32 devices in a mesh: sp: 8 (over z, y), tp: 4 (over x, core).
Axes of the slice: x: 2, y: 2, z: 4, core: 2. Of those that a mesh axis runs over, the one named last changes fastest.
Arguments:
- residual: bfloat16 [5120, 2048], P('sp', 'tp'), may hold values from -4 to 4
- query_wide: bfloat16 [5120, 1536], P('sp', 'tp'), may hold values from -500 to 500
- query_narrow: bfloat16 [5120, 1024], P('sp', 'tp'), may hold values from -500 to 500
- latent: bfloat16 [5120, 512], P('sp'), may hold values from -6 to 6
- rope_key: bfloat16 [5120, 64], P('sp'), may hold values from -6 to 6
- latent_gain: float32 [512], replicated, may hold values from 0.1 to 1.9
- expand_wide: bfloat16 [512, 2048], P(None, 'tp'), may hold values from -0.25 to 0.25
- expand_narrow: bfloat16 [512, 1024], P(None, 'tp'), may hold values from -0.25 to 0.25
- out_wide: bfloat16 [1024, 2048], P('tp'), may hold values from -0.1875 to 0.1875
- out_narrow: bfloat16 [512, 2048], P('tp'), may hold values from -0.25 to 0.25
- norm_gain: float32 [2048], P('tp'), may hold values from 0.1 to 1.9
- up_gate: bfloat16 [2048, 5632], P('sp', 'tp'), may hold values from -0.125 to 0.125
- up_value: bfloat16 [2048, 5632], P('sp', 'tp'), may hold values from -0.125 to 0.125
- down_weight: bfloat16 [2048, 5632], P('sp', 'tp'), may hold values from -0.078125 to 0.078125
- conv_taps: float32 [3, 2, 5632], P(None, None, 'tp'), may hold values from -3 to 3
Outputs:
- output: bfloat16 [5120, 2048], P('sp', 'tp')
The draws below stay inside these ranges and needn't reach their ends.
All inputs are finite; a program needn't handle non-finite values.
Results may differ from the reference program's by a relative error of at most 0.025.
Values may be sent and summed in bfloat16 or wider, within the bound.
No kernel may reach another device: no remote copies, remote signals or barrier semaphores. Data moves between devices by JAX's collectives and lax.ppermute only.
A program may use at most 192 MiB of HBM per device.

```python
import math
import jax
import jax.numpy as jnp
from jax import lax

D = 2048
FF = 5632
RANK = 512
ROPE = 64
HW = 8
NOPE_W = 128
VAL_W = 128
HN = 8
NOPE_N = 64
VAL_N = 64
TOKENS = 5120
N_TP = 4


def draw_residual(key, part):
    key_noise = jax.random.fold_in(key, 11)
    columns = jnp.arange(D, dtype=jnp.float32) / D
    values = jax.random.normal(key_noise, (TOKENS, D), jnp.float32) * 0.1 * jnp.exp(1.6 * columns)[None, :]
    return jnp.clip(values, -4.0, 4.0).astype(jnp.bfloat16)


def query_values(key, arr_shape):
    key_noise = jax.random.fold_in(key, 21)
    values = jax.random.normal(key_noise, arr_shape, jnp.float32) * 2.5
    return jnp.clip(values, -12.0, 12.0)


def draw_query_wide(key, part):
    return query_values(jax.random.fold_in(key, 1), (TOKENS, HW * (NOPE_W + ROPE))).astype(jnp.bfloat16)


def draw_query_narrow(key, part):
    return query_values(jax.random.fold_in(key, 2), (TOKENS, HN * (NOPE_N + ROPE))).astype(jnp.bfloat16)


def level_of(key, dims, cuts, smallest, high):
    gain = 1.0
    for dim, blocks in cuts:
        draws = jax.random.uniform(jax.random.fold_in(jax.random.fold_in(key, 6), dim), (blocks,), jnp.float32, smallest / len(cuts), high / len(cuts))
        gain = gain * jnp.repeat(jnp.exp(draws), dims[dim] // blocks).reshape((-1,) + (1,) * (len(dims) - 1 - dim))
    return gain


def scatter_about(key, extent, scale, reach, cuts=(), kind=jnp.bfloat16):
    level = level_of(key, extent, cuts, -0.22, 0.18) if cuts else 1.0
    values = jax.random.normal(key, extent, jnp.float32) * scale * level
    return jnp.minimum(jnp.maximum(values, -reach), reach).astype(kind)


def setup_inputs(seed: int = 0) -> dict:
    arg_keys = jax.random.split(jax.random.key(seed), 16)
    return {
        "residual": draw_residual(jax.random.fold_in(arg_keys[15], 71), 0),
        "query_wide": draw_query_wide(jax.random.fold_in(arg_keys[15], 71), 0),
        "query_narrow": draw_query_narrow(jax.random.fold_in(arg_keys[15], 71), 0),
        "latent": scatter_about(arg_keys[3], (TOKENS, RANK), 1.0, 6.0, ((0, 8),)),
        "rope_key": scatter_about(arg_keys[4], (TOKENS, ROPE), 1.0, 6.0, ((0, 8),)),
        "latent_gain": jnp.clip(1.0 + 0.18 * jax.random.normal(arg_keys[5], (RANK,), jnp.float32), 0.1, 1.9),
        "expand_wide": scatter_about(arg_keys[6], (RANK, HW * (NOPE_W + VAL_W)), RANK ** -0.5, 0.25, ((1, 4),)),
        "expand_narrow": scatter_about(arg_keys[7], (RANK, HN * (NOPE_N + VAL_N)), RANK ** -0.5, 0.25, ((1, 4),)),
        "out_wide": scatter_about(arg_keys[8], (HW * VAL_W, D), (HW * VAL_W) ** -0.5, 0.1875, ((0, 4),)),
        "out_narrow": scatter_about(arg_keys[9], (HN * VAL_N, D), (HN * VAL_N) ** -0.5, 0.25, ((0, 4),)),
        "norm_gain": jnp.clip(1.0 + 0.18 * jax.random.normal(arg_keys[10], (D,), jnp.float32), 0.1, 1.9),
        "up_gate": scatter_about(arg_keys[11], (D, FF), D ** -0.5, 0.125, ((0, 8), (1, 4))),
        "up_value": scatter_about(arg_keys[12], (D, FF), D ** -0.5, 0.125, ((0, 8), (1, 4))),
        "down_weight": scatter_about(arg_keys[13], (D, FF), FF ** -0.5, 0.078125, ((0, 8), (1, 4))),
        "conv_taps": scatter_about(arg_keys[14], (3, 2, FF), 0.6, 3.0, ((2, 4),), jnp.float32),
    }


theta = 10000.0
epsilon = 1e-06

def rotate(values, positions):
    half_dim = values.shape[-1] // 2
    inverse = jnp.power(jnp.float32(theta), -2.0 * jnp.arange(half_dim, dtype=jnp.float32) / values.shape[-1])
    angles = positions[:, None] * inverse[None, :]
    new_shape = (angles.shape[0],) + (1,) * (values.ndim - 2) + (half_dim,)
    cosine = jnp.cos(angles).reshape(new_shape)
    sine_part = jnp.sin(angles).reshape(new_shape)
    floats = values.astype(jnp.float32)
    lower_half = floats[..., :half_dim]
    upper_half = floats[..., half_dim:]
    turned = jnp.concatenate([lower_half * cosine - upper_half * sine_part, lower_half * sine_part + upper_half * cosine], axis=-1)
    return turned.astype(jnp.bfloat16)

def attend(query_turned, key_part, value_part, rope_turned, factor):
    nope_dim = key_part.shape[-1]
    head_count = query_turned.shape[1]
    block_rows = math.gcd(TOKENS, 512)
    grouped = query_turned.reshape(TOKENS // block_rows, block_rows, head_count, query_turned.shape[-1])
    key_float = key_part.astype(jnp.float32)
    rope_float = rope_turned.astype(jnp.float32)
    value_float = value_part.astype(jnp.float32)

    def one_block(query_block):
        query_float = query_block.astype(jnp.float32)
        scores = jnp.einsum('qhd,khd->hqk', query_float[..., :nope_dim], key_float)
        scores = (scores + jnp.einsum('qhd,kd->hqk', query_float[..., nope_dim:], rope_float)) * factor
        row_max = lax.optimization_barrier(jnp.max(scores, axis=-1, keepdims=True))
        weights = jnp.exp(scores - row_max)
        row_total = lax.optimization_barrier(jnp.sum(weights, axis=-1))
        rounded = lax.optimization_barrier(weights.astype(jnp.bfloat16)).astype(jnp.float32)
        weighted = jnp.einsum('hqk,khd->qhd', rounded, value_float)
        return (weighted / jnp.transpose(row_total)[:, :, None]).astype(jnp.bfloat16)
    outputs = lax.map(one_block, grouped)
    return outputs.reshape(TOKENS, head_count * value_part.shape[-1])

def turn_query(queries, head_count, nope_dim, positions):
    shaped = queries.reshape(TOKENS, head_count, nope_dim + ROPE)
    return jnp.concatenate([shaped[..., :nope_dim], rotate(shaped[..., nope_dim:], positions)], axis=-1)

def convolve(values, tap_rows):
    floats = values.astype(jnp.float32)
    zero_row = jnp.zeros((1, floats.shape[1]), jnp.float32)
    before = jnp.concatenate([zero_row, floats[:-1]], axis=0)
    after = jnp.concatenate([floats[1:], zero_row], axis=0)
    return tap_rows[0] * before + tap_rows[1] * floats + tap_rows[2] * after

def reference(residual, query_wide, query_narrow, latent, rope_key, latent_gain, expand_wide, expand_narrow, out_wide, out_narrow, norm_gain, up_gate, up_value, down_weight, conv_taps):
    positions = jnp.arange(TOKENS, dtype=jnp.int32).astype(jnp.float32)
    latent_float = latent.astype(jnp.float32)
    normed_latent = (latent_float * lax.rsqrt(lax.optimization_barrier(jnp.mean(latent_float * latent_float, axis=-1, keepdims=True)) + epsilon) * latent_gain).astype(jnp.bfloat16)
    rope_turned = rotate(rope_key, positions)
    kv_wide = jnp.dot(normed_latent, expand_wide, preferred_element_type=jnp.float32).astype(jnp.bfloat16).reshape(TOKENS, HW, NOPE_W + VAL_W)
    kv_narrow = jnp.dot(normed_latent, expand_narrow, preferred_element_type=jnp.float32).astype(jnp.bfloat16).reshape(TOKENS, HN, NOPE_N + VAL_N)
    query_w = turn_query(query_wide, HW, NOPE_W, positions)
    query_n = turn_query(query_narrow, HN, NOPE_N, positions)
    heads_wide = attend(query_w, kv_wide[..., :NOPE_W], kv_wide[..., NOPE_W:], rope_turned, (NOPE_W + ROPE) ** (-0.5))
    heads_narrow = attend(query_n, kv_narrow[..., :NOPE_N], kv_narrow[..., NOPE_N:], rope_turned, (NOPE_N + ROPE) ** (-0.5))
    wide_cols = HW // N_TP * VAL_W
    narrow_cols = HN // N_TP * VAL_N
    projected = jnp.zeros((TOKENS, D), jnp.float32)
    for group_index in range(N_TP):
        wide_slice = slice(group_index * wide_cols, (group_index + 1) * wide_cols)
        narrow_slice = slice(group_index * narrow_cols, (group_index + 1) * narrow_cols)
        partial_value = jnp.dot(heads_wide[:, wide_slice], out_wide[wide_slice], preferred_element_type=jnp.float32)
        partial_value = partial_value + jnp.dot(heads_narrow[:, narrow_slice], out_narrow[narrow_slice], preferred_element_type=jnp.float32)
        projected = projected + lax.optimization_barrier(partial_value.astype(jnp.bfloat16)).astype(jnp.float32)
    attended = (residual.astype(jnp.float32) + projected).astype(jnp.bfloat16)
    attended_float = attended.astype(jnp.float32)
    factor_rows = lax.rsqrt(lax.optimization_barrier(jnp.mean(attended_float * attended_float, axis=-1, keepdims=True)) + epsilon)
    normed = (attended_float * factor_rows * norm_gain).astype(jnp.bfloat16)
    gate_up = jnp.dot(normed, up_gate, preferred_element_type=jnp.float32).astype(jnp.bfloat16)
    value_up = jnp.dot(normed, up_value, preferred_element_type=jnp.float32).astype(jnp.bfloat16)
    hidden = (jax.nn.silu(convolve(gate_up, conv_taps[:, 0])) * convolve(value_up, conv_taps[:, 1])).astype(jnp.bfloat16)
    unit_cols = FF // N_TP
    channels = jnp.zeros((TOKENS, D), jnp.float32)
    for group_index in range(N_TP):
        unit_slice = slice(group_index * unit_cols, (group_index + 1) * unit_cols)
        partial_value = lax.dot_general(hidden[:, unit_slice], down_weight[:, unit_slice], (((1,), (1,)), ((), ())), preferred_element_type=jnp.float32)
        channels = channels + lax.optimization_barrier(partial_value.astype(jnp.bfloat16)).astype(jnp.float32)
    return (attended_float + channels).astype(jnp.bfloat16)
```

```python
import functools

import jax
import jax.numpy as jnp
from jax import lax
from jax.experimental import pallas as pl
from jax.experimental.pallas import tpu as pltpu
from jax.sharding import PartitionSpec as P


D = 2048
ROPE = 64
NOPE_W = 128
VAL_W = 128
NOPE_N = 64
VAL_N = 64
LANES = 128

theta = 10000.0
epsilon = 1e-06
F32 = jnp.float32
BF16 = jnp.bfloat16
LOG2E = 1.4426950408889634


def rotate(values, positions):
    half_dim = values.shape[-1] // 2
    inverse = jnp.power(
        jnp.float32(theta), -2.0 * jnp.arange(half_dim, dtype=jnp.float32) / values.shape[-1]
    )
    angles = positions[:, None] * inverse[None, :]
    new_shape = (angles.shape[0],) + (1,) * (values.ndim - 2) + (half_dim,)
    cosine = jnp.cos(angles).reshape(new_shape)
    sine_part = jnp.sin(angles).reshape(new_shape)
    floats = values.astype(jnp.float32)
    lower_half = floats[..., :half_dim]
    upper_half = floats[..., half_dim:]
    turned = jnp.concatenate(
        [
            lower_half * cosine - upper_half * sine_part,
            lower_half * sine_part + upper_half * cosine,
        ],
        axis=-1,
    )
    return turned.astype(jnp.bfloat16)


def up_to(width, unit=LANES):
    return -(-width // unit) * unit


def turn_query(queries, head_count, nope_dim, positions):
    shaped = queries.reshape(queries.shape[0], head_count, nope_dim + ROPE)
    width = nope_dim + ROPE
    parts = [shaped[..., :nope_dim], rotate(shaped[..., nope_dim:], positions)]
    if up_to(width) > width:
        parts.append(jnp.zeros(shaped.shape[:2] + (up_to(width) - width,), BF16))
    return jnp.concatenate(parts, axis=-1).reshape(queries.shape[0], -1)


def expansion(expand, heads, nope_dim, value_dim):
    rank = expand.shape[0]
    shaped = expand.reshape(rank, heads, nope_dim + value_dim)
    width = up_to(nope_dim + ROPE)
    key_top = jnp.pad(shaped[..., :nope_dim], ((0, 0), (0, 0), (0, width - nope_dim)))
    eye = jnp.pad(jnp.eye(ROPE, dtype=BF16), ((0, 0), (nope_dim, width - nope_dim - ROPE)))
    key_low = jnp.broadcast_to(eye[:, None, :], (ROPE, heads, width))
    keys = jnp.concatenate([key_top, key_low], axis=0).reshape(rank + ROPE, heads * width)
    values = shaped[..., nope_dim:].reshape(rank, heads * value_dim)
    values = jnp.pad(values, ((0, ROPE), (0, up_to(heads * value_dim) - heads * value_dim)))
    return jnp.concatenate([keys, values], axis=1)


def attention_kernel(heads, width, value_dim, factor, rows, tile, q_ref, kv_ref, o_ref, s_scr, m_scr, l_scr, a_scr):
    blocks = q_ref.shape[0] // rows
    key_count = kv_ref.shape[0]
    tiles = key_count // tile
    groups = tile // LANES
    scale = factor * LOG2E
    value_base = heads * width
    total = heads * blocks

    def place(b):
        h = b // blocks
        r = pl.multiple_of((b - h * blocks) * rows, rows)
        return h, r

    def score(b, buf, j):
        h, r = place(b)
        q = q_ref[pl.ds(r, rows), pl.ds(pl.multiple_of(h * width, LANES), width)]
        at = pl.multiple_of(j * tile, tile)
        k = kv_ref[pl.ds(at, tile), pl.ds(pl.multiple_of(h * width, LANES), width)]
        s = lax.dot_general(q, k, (((1,), (1,)), ((), ())), preferred_element_type=F32)
        s_scr[buf, :, pl.ds(at, tile)] = s
        top = s[:, :LANES]
        for g in range(1, groups):
            top = jnp.maximum(top, s[:, g * LANES : (g + 1) * LANES])
        m_scr[buf] = jnp.maximum(m_scr[buf], top)

    def clear_max(buf):
        m_scr[buf] = jnp.full((rows, LANES), -jnp.inf, F32)

    def settle_max(buf):
        top = jnp.max(m_scr[buf], axis=1, keepdims=True)
        m_scr[buf] = jnp.broadcast_to(top, (rows, LANES))

    def weigh(b, buf, j):
        h, r = place(b)
        at = pl.multiple_of(j * tile, tile)
        v_at = pl.multiple_of(value_base + (h * value_dim) // LANES * LANES, LANES)
        v = kv_ref[pl.ds(at, tile), pl.ds(v_at, LANES)]
        top = m_scr[buf]
        low = []
        part = None
        for g in range(groups):
            s = s_scr[buf, :, pl.ds(pl.multiple_of(at + g * LANES, LANES), LANES)]
            p = jnp.exp2((s - top) * scale)
            part = p if part is None else part + p
            low.append(p.astype(BF16))
        l_scr[...] += part
        a_scr[...] += jnp.dot(jnp.concatenate(low, axis=1), v, preferred_element_type=F32)

    def write(b):
        h, r = place(b)
        out = (a_scr[...] / jnp.sum(l_scr[...], axis=1, keepdims=True)).astype(BF16)
        at = pl.multiple_of((h * value_dim) // LANES * LANES, LANES)
        if value_dim % LANES == 0:
            o_ref[pl.ds(r, rows), pl.ds(at, LANES)] = out
        else:
            lane = lax.broadcasted_iota(jnp.int32, (rows, LANES), 1)
            start = h * value_dim - at
            mine = (lane >= start) & (lane < start + value_dim)
            old = o_ref[pl.ds(r, rows), pl.ds(at, LANES)]
            o_ref[pl.ds(r, rows), pl.ds(at, LANES)] = jnp.where(mine, out, old)

    if value_dim % LANES:
        o_ref[...] = jnp.zeros_like(o_ref)
    clear_max(0)

    def first(j, c):
        score(0, 0, j)
        return c

    lax.fori_loop(0, tiles, first, 0)

    def step(b, c):
        buf = lax.rem(b, 2)
        settle_max(buf)
        clear_max(1 - buf)
        l_scr[...] = jnp.zeros_like(l_scr)
        a_scr[...] = jnp.zeros_like(a_scr)
        after = jnp.minimum(b + 1, total - 1)

        def both(j, c):
            score(after, 1 - buf, j)
            weigh(b, buf, j)
            return c

        lax.fori_loop(0, tiles, both, 0)
        write(b)
        return c

    lax.fori_loop(0, total, step, 0)


def attend(query, kv, heads, width, value_dim, factor):
    rows = 128 if query.shape[0] % 128 == 0 else query.shape[0]
    tile = 1024 if kv.shape[0] % 1024 == 0 else kv.shape[0]
    out_width = up_to(heads * value_dim)
    flops = 2 * query.shape[0] * kv.shape[0] * heads * (width + LANES)
    out = pl.pallas_call(
        functools.partial(attention_kernel, heads, width, value_dim, factor, rows, tile),
        out_shape=jax.ShapeDtypeStruct((query.shape[0], out_width), BF16),
        in_specs=[pl.BlockSpec(memory_space=pltpu.VMEM)] * 2,
        out_specs=pl.BlockSpec(memory_space=pltpu.VMEM),
        scratch_shapes=[
            pltpu.VMEM((2, rows, kv.shape[0]), F32),
            pltpu.VMEM((2, rows, LANES), F32),
            pltpu.VMEM((rows, LANES), F32),
            pltpu.VMEM((rows, LANES), F32),
        ],
        compiler_params=pltpu.CompilerParams(vmem_limit_bytes=40 * 2**20),
        cost_estimate=pl.CostEstimate(
            flops=flops * 8, bytes_accessed=kv.size * 2, transcendentals=query.shape[0] * kv.shape[0] * heads
        ),
        name="attend",
    )(query, kv)
    return out[:, : heads * value_dim]


def per_device(
    sp_size,
    tp_size,
    residual,
    query_wide,
    query_narrow,
    latent,
    rope_key,
    latent_gain,
    expand_wide,
    expand_narrow,
    out_wide,
    out_narrow,
    norm_gain,
    up_gate,
    up_value,
    down_weight,
    conv_taps,
):
    ring = sp_size // 2
    me = lax.axis_index("sp")
    tp = lax.axis_index("tp")
    side = lax.rem(me, 2)
    core = lax.rem(tp, 2)
    tok_rows = residual.shape[0]
    positions = (me * tok_rows + lax.iota(jnp.int32, tok_rows)).astype(jnp.float32)

    def mate(a):
        return lax.ppermute(a, "sp", [(i, i ^ 1) for i in range(sp_size)])

    def along(a, k):
        return lax.ppermute(a, "sp", [(i, (i + 2 * k) % sp_size) for i in range(sp_size)])

    def across(a, bit):
        return lax.ppermute(a, "tp", [(i, i ^ bit) for i in range(tp_size)])

    far_bits = []
    bit = 2
    while bit < tp_size:
        far_bits.append(bit)
        bit *= 2
    tp_order = [0]
    for bit in far_bits + [1]:
        tp_order = tp_order + [p ^ bit for p in tp_order]

    def over_tp(a, axis):
        for bit in far_bits + [1]:
            a = jnp.concatenate([a, across(a, bit)], axis=axis)
        return a

    def paired(own, other):
        return jnp.where(side == 0, jnp.concatenate([own, other]), jnp.concatenate([other, own]))

    units = up_gate.shape[1]
    half = units // 2

    def halves(gate, value, down):
        low = (gate[:, :half], value[:, :half], down[:, :half])
        high = (gate[:, half:], value[:, half:], down[:, half:])
        keep = [jnp.where(side == 0, a, b) for a, b in zip(low, high)]
        give = [jnp.where(side == 0, b, a) for a, b in zip(low, high)]
        return keep, give

    keep, give = halves(up_gate, up_value, down_weight)
    up_keep = jnp.concatenate(keep[:2], axis=1)
    up_give = jnp.concatenate(give[:2], axis=1)

    latent_float = latent.astype(F32)
    normed_latent = (
        latent_float
        * lax.rsqrt(jnp.mean(latent_float * latent_float, axis=-1, keepdims=True) + epsilon)
        * latent_gain
    ).astype(BF16)
    packed = jnp.concatenate([normed_latent, rotate(rope_key, positions)], axis=1)
    core_rows = tok_rows // 2
    mine = lax.dynamic_slice_in_dim(packed, core * core_rows, core_rows, axis=0)
    hops = [along(mine, k) for k in range(1, ring)]
    up_mate = mate(up_give)
    sides = [mate(mine)] + [mate(h) for h in hops]
    remote = jnp.concatenate(hops + sides, axis=0)
    latents = jnp.concatenate([packed, remote, across(remote, 1)], axis=0)

    up_a, up_b = [up_keep], [up_mate]
    down_mate = mate(give[2])
    down_a, down_b = [keep[2]], [down_mate]
    for k in range(1, ring):
        up_a.append(along(up_a[-1], 1))
        up_b.append(along(up_b[-1], 1))
    for k in range(1, ring):
        down_a.append(along(down_a[-1], 1))
        down_b.append(along(down_b[-1], 1))

    outs = over_tp(jnp.concatenate([out_wide, out_narrow], axis=0), 0)
    out_rows = out_wide.shape[0] + out_narrow.shape[0]
    wide_rows = out_wide.shape[0]
    outs = outs.reshape(tp_size, out_rows, outs.shape[1])
    out_w = outs[:, :wide_rows].reshape(-1, outs.shape[2])
    out_n = outs[:, wide_rows:].reshape(-1, outs.shape[2])
    own_width = residual.shape[1]
    pair_residual = paired(residual, mate(residual))
    spread = over_tp(pair_residual, 1)
    gains = over_tp(norm_gain[None, :], 1)
    full_residual = jnp.zeros((2 * tok_rows, own_width * tp_size), BF16)
    full_gain = jnp.zeros((1, own_width * tp_size), F32)
    for p, q in enumerate(tp_order):
        at = jnp.bitwise_xor(tp, q) * own_width
        piece = slice(p * own_width, (p + 1) * own_width)
        full_residual = lax.dynamic_update_slice_in_dim(full_residual, spread[:, piece], at, axis=1)
        full_gain = lax.dynamic_update_slice_in_dim(full_gain, gains[:, piece], at, axis=1)

    wide_heads = query_wide.shape[1] // (NOPE_W + ROPE)
    narrow_heads = query_narrow.shape[1] // (NOPE_N + ROPE)
    query_w = turn_query(query_wide, wide_heads, NOPE_W, positions)
    query_n = turn_query(query_narrow, narrow_heads, NOPE_N, positions)
    kv_w = jnp.dot(
        latents, expansion(expand_wide, wide_heads, NOPE_W, VAL_W), preferred_element_type=F32
    ).astype(BF16)
    kv_n = jnp.dot(
        latents, expansion(expand_narrow, narrow_heads, NOPE_N, VAL_N), preferred_element_type=F32
    ).astype(BF16)
    heads_w = attend(query_w, kv_w, wide_heads, up_to(NOPE_W + ROPE), VAL_W, (NOPE_W + ROPE) ** (-0.5))
    heads_n = attend(query_n, kv_n, narrow_heads, up_to(NOPE_N + ROPE), VAL_N, (NOPE_N + ROPE) ** (-0.5))
    full_w = over_tp(paired(heads_w, mate(heads_w)), 1)
    full_n = over_tp(paired(heads_n, mate(heads_n)), 1)
    projected = jnp.dot(full_w, out_w, preferred_element_type=F32)
    projected = projected + jnp.dot(full_n, out_n, preferred_element_type=F32)
    attended = (full_residual.astype(F32) + projected).astype(BF16)
    attended_float = attended.astype(F32)
    factor_rows = lax.rsqrt(jnp.mean(attended_float * attended_float, axis=-1, keepdims=True) + epsilon)
    normed = (attended_float * factor_rows * full_gain).astype(BF16)

    block = up_gate.shape[0]
    position = me // 2
    both = None
    for k in range(ring):
        source = lax.rem(position - k + ring, ring) * 2
        own_at = (source + side) * block
        mate_at = (source + 1 - side) * block
        for at, piece in ((own_at, up_a[k]), (mate_at, up_b[k])):
            part = jnp.dot(
                lax.dynamic_slice_in_dim(normed, at, block, axis=1), piece, preferred_element_type=F32
            )
            both = part if both is None else both + part
    both = both.astype(BF16)
    up_line = [(i, i + 2) for i in range(sp_size - 2)]
    low = lax.ppermute(both[-1:], "sp", up_line)
    high = lax.ppermute(both[:1], "sp", [(b, a) for a, b in up_line])
    extended = jnp.concatenate([low, both, high], axis=0).astype(F32)
    taps = jnp.where(side == 0, conv_taps[:, :, :half], conv_taps[:, :, half:])
    taps = taps.reshape(3, 2 * half)
    smoothed = taps[0] * extended[:-2] + taps[1] * extended[1:-1] + taps[2] * extended[2:]
    hidden = (jax.nn.silu(smoothed[:, :half]) * smoothed[:, half:]).astype(BF16)

    terms = jnp.zeros((2 * tok_rows, block * sp_size), BF16)
    for k in range(ring):
        source = lax.rem(position - k + ring, ring) * 2
        own_at = (source + side) * block
        mate_at = (source + 1 - side) * block
        for at, piece in ((own_at, down_a[k]), (mate_at, down_b[k])):
            part = lax.dot_general(
                hidden, piece, (((1,), (1,)), ((), ())), preferred_element_type=F32
            ).astype(BF16)
            terms = lax.dynamic_update_slice_in_dim(terms, part, at, axis=1)

    blocks = terms.reshape(2 * tok_rows, tp_size, own_width)
    width = tp_size
    for bit in [1] + far_bits[::-1]:
        width //= 2
        split = tp_size // (2 * bit) if bit > 1 else tp_size // 2
        if bit == 1:
            shaped = blocks.reshape(2 * tok_rows, tp_size // 2, 2, own_width)
            even, odd = shaped[:, :, 0], shaped[:, :, 1]
        else:
            even, odd = blocks[:, :width], blocks[:, width:]
        on = (tp // bit) % 2
        kept = jnp.where(on == 0, even, odd)
        sent = jnp.where(on == 0, odd, even)
        got = across(sent, bit)
        blocks = (kept.astype(F32) + got.astype(F32)).astype(BF16)
    summed = blocks.reshape(2 * tok_rows, own_width)
    kept = lax.dynamic_slice_in_dim(summed, side * tok_rows, tok_rows, axis=0)
    sent = lax.dynamic_slice_in_dim(summed, (1 - side) * tok_rows, tok_rows, axis=0)
    got = mate(sent)
    own = lax.dynamic_slice(
        attended, (side * tok_rows, tp * own_width), (tok_rows, own_width)
    )
    return (own.astype(F32) + (kept.astype(F32) + got.astype(F32))).astype(BF16)


def solution(mesh):
    in_specs = (
        P("sp", "tp"),
        P("sp", "tp"),
        P("sp", "tp"),
        P("sp", None),
        P("sp", None),
        P(),
        P(None, "tp"),
        P(None, "tp"),
        P("tp", None),
        P("tp", None),
        P("tp"),
        P("sp", "tp"),
        P("sp", "tp"),
        P("sp", "tp"),
        P(None, None, "tp"),
    )
    out_specs = P("sp", "tp")
    body = functools.partial(per_device, mesh.shape["sp"], mesh.shape["tp"])
    return jax.shard_map(body, mesh=mesh, in_specs=in_specs, out_specs=out_specs, check_vma=False)
```

```python
import functools

import jax
import jax.numpy as jnp
from jax import lax
from jax.experimental import pallas as pl
from jax.experimental.pallas import tpu as pltpu
from jax.sharding import PartitionSpec as P


ROPE = 64
NOPE_W = 128
VAL_W = 128
NOPE_N = 64
VAL_N = 64
LANES = 128

theta = 10000.0
epsilon = 1e-06
F32 = jnp.float32
BF16 = jnp.bfloat16
LOG2E = 1.4426950408889634


def angles_of(positions):
    half_dim = ROPE // 2
    inverse = jnp.power(jnp.float32(theta), -2.0 * jnp.arange(half_dim, dtype=jnp.float32) / ROPE)
    angles = positions[:, None] * inverse[None, :]
    return jnp.cos(angles), jnp.sin(angles)


def rotate(values, cosine, sine):
    half_dim = values.shape[-1] // 2
    floats = values.astype(jnp.float32)
    lower_half = floats[..., :half_dim]
    upper_half = floats[..., half_dim:]
    turned = jnp.concatenate(
        [
            lower_half * cosine - upper_half * sine,
            lower_half * sine + upper_half * cosine,
        ],
        axis=-1,
    )
    return turned.astype(jnp.bfloat16)


def gather_in(pieces, target, offsets, sems):
    copies = []
    for i, (piece, at) in enumerate(zip(pieces, offsets)):
        copy = pltpu.make_async_copy(piece, target.at[pl.ds(at, piece.shape[0])], sems.at[i])
        copy.start()
        copies.append(copy)
    return copies


def attention_kernel(wide, heads, odd, pick, factor, rows, tile, passes, *refs):
    scratch = 10 if passes else 9
    q_ref, c_ref, n_ref, e_ref, *pieces = refs[:-scratch]
    o_ref, lat, q_scr, kv_ref, s_scr, m_scr, l_scr, a_scr, sems = (refs[-10:-9] + refs[-8:]) if passes else refs[-9:]
    width = q_scr.shape[1] // heads
    blocks = q_ref.shape[0] // rows
    key_count = kv_ref.shape[0]
    rank = e_ref.shape[0]
    tiles = key_count // tile
    groups = tile // LANES
    scale = factor * LOG2E
    value_base = heads * width
    total = heads * blocks

    def fetch(j):
        at = pl.ds(pl.multiple_of(j * tile, tile), tile)
        return pltpu.make_async_copy(pieces[0].at[at], lat.at[at], sems.at[j])

    offsets, at = [], 0
    for piece in pieces:
        offsets.append(at)
        at += piece.shape[0]
    if len(pieces) > 1:
        copies = gather_in(pieces, lat, offsets, sems)
    else:
        copies = []
        for j in range(tiles):
            fetch(j).start()

    def turn(values):
        lane = lax.broadcasted_iota(jnp.int32, values.shape, 1)
        quarter = ROPE // 2
        swapped = jnp.where(
            (lane // quarter) % 2 == 0,
            pltpu.roll(values, LANES - quarter, 1),
            pltpu.roll(values, quarter, 1),
        )
        return (values * c_ref[...] + swapped * n_ref[...]).astype(BF16)

    queries = q_ref[...].astype(F32)
    for h in range(heads):
        if wide:
            head = NOPE_W + ROPE
            full = queries.shape[1]
            if full < 2 * LANES:
                shifted = jnp.concatenate([queries, jnp.zeros((queries.shape[0], 2 * LANES - full), F32)], axis=1)
            else:
                shifted = queries if h + pick == 0 else pltpu.roll(queries, full - (h + pick) * head, 1)
            q_scr[:, h * width : h * width + LANES] = shifted[:, :LANES].astype(BF16)
            q_scr[:, h * width + LANES : (h + 1) * width] = turn(shifted[:, LANES : 2 * LANES])
        else:
            q_scr[:, h * width : (h + 1) * width] = turn(queries[:, h * width : (h + 1) * width])

    for copy in copies:
        copy.wait()
    if passes:
        onward = pltpu.make_async_copy(lat, refs[-9], sems.at[len(pieces)])
        onward.start()

    def expand(j, c):
        at = pl.multiple_of(j * tile, tile)
        if not copies:
            fetch(j).wait()
        x = lat[pl.ds(at, tile), :rank]
        rope = lat[pl.ds(at, tile), rank:].astype(F32)
        lane = lax.broadcasted_iota(jnp.int32, rope.shape, 1)
        for h in range(heads):
            if wide:
                both = NOPE_W + VAL_W
                kv = jnp.dot(x, e_ref[:, (h + pick) * both : (h + pick + 1) * both], preferred_element_type=F32).astype(BF16)
                kv_ref[pl.ds(at, tile), h * width : h * width + LANES] = kv[:, :LANES]
                kv_ref[pl.ds(at, tile), h * width + LANES : (h + 1) * width] = jnp.where(
                    lane < ROPE, rope, 0.0
                ).astype(BF16)
                v_at = value_base + h * LANES
                kv_ref[pl.ds(at, tile), v_at : v_at + LANES] = kv[:, LANES:]
            else:
                kv = jnp.dot(x, e_ref[...], preferred_element_type=F32)
                kv_ref[pl.ds(at, tile), :LANES] = jnp.where(lane < NOPE_N, kv, rope).astype(BF16)
                kv_ref[pl.ds(at, tile), LANES:] = kv.astype(BF16)
        return c

    lax.fori_loop(0, tiles, expand, 0)

    def place(b):
        h = b // blocks
        return h, pl.multiple_of((b - h * blocks) * rows, rows)

    def score(b, buf, j):
        h, r = place(b)
        q = q_scr[pl.ds(r, rows), pl.ds(pl.multiple_of(h * width, LANES), width)]
        at = pl.multiple_of(j * tile, tile)
        k = kv_ref[pl.ds(at, tile), pl.ds(pl.multiple_of(h * width, LANES), width)]
        s = lax.dot_general(q, k, (((1,), (1,)), ((), ())), preferred_element_type=F32)
        s_scr[buf, :, pl.ds(at, tile)] = s
        top = s[:, :LANES]
        for g in range(1, groups):
            top = jnp.maximum(top, s[:, g * LANES : (g + 1) * LANES])
        m_scr[buf] = jnp.maximum(m_scr[buf], top)

    def weigh(b, buf, j):
        h, _ = place(b)
        at = pl.multiple_of(j * tile, tile)
        v_at = pl.multiple_of(value_base + h * LANES, LANES)
        v = kv_ref[pl.ds(at, tile), pl.ds(v_at, LANES)]
        top = m_scr[buf]
        low = []
        part = None
        for g in range(groups):
            s = s_scr[buf, :, pl.ds(pl.multiple_of(at + g * LANES, LANES), LANES)]
            p = jnp.exp2((s - top) * scale)
            part = p if part is None else part + p
            low.append(p.astype(BF16))
        l_scr[...] += part
        a_scr[...] += jnp.dot(jnp.concatenate(low, axis=1), v, preferred_element_type=F32)

    def write(b):
        h, r = place(b)
        out = a_scr[...] / jnp.sum(l_scr[...], axis=1, keepdims=True)
        if not wide:
            lane = lax.broadcasted_iota(jnp.int32, (rows, LANES), 1)
            if odd:
                out = jnp.where(lane >= VAL_N, out, 0.0)
            else:
                out = jnp.where(lane < VAL_N, pltpu.roll(out, VAL_N, 1), 0.0)
        o_ref[pl.ds(r, rows), pl.ds(pl.multiple_of(h * LANES, LANES), LANES)] = out.astype(BF16)

    def clear_max(buf):
        m_scr[buf] = jnp.full((rows, LANES), -jnp.inf, F32)

    clear_max(0)

    def first(j, c):
        score(0, 0, j)
        return c

    lax.fori_loop(0, tiles, first, 0)

    def step(b, c):
        buf = lax.rem(b, 2)
        m_scr[buf] = jnp.broadcast_to(jnp.max(m_scr[buf], axis=1, keepdims=True), (rows, LANES))
        clear_max(1 - buf)
        l_scr[...] = jnp.zeros_like(l_scr)
        a_scr[...] = jnp.zeros_like(a_scr)
        after = jnp.minimum(b + 1, total - 1)

        def both(j, c):
            score(after, 1 - buf, j)
            weigh(b, buf, j)
            return c

        lax.fori_loop(0, tiles, both, 0)
        write(b)
        return c

    lax.fori_loop(0, total, step, 0)
    if passes:
        onward.wait()


VMEM_SPEC = pl.BlockSpec(memory_space=pltpu.VMEM)
SMEM_SPEC = pl.BlockSpec(memory_space=pltpu.SMEM)
HBM_SPEC = pl.BlockSpec(memory_space=pltpu.HBM)
ANY_SPEC = pl.BlockSpec(memory_space=pl.ANY)


def attend(query, tables, weights, pieces, heads, wide, odd, factor, passes=False, pick=0):
    tok = query.shape[0]
    keys = sum(p.shape[0] for p in pieces)
    rows = tok // 2 if tok % 32 == 0 else tok
    tile = 1024 if keys % 1024 == 0 else keys
    width = 2 * LANES if wide else LANES
    out = jax.ShapeDtypeStruct((tok, heads * LANES), BF16)
    kept = jax.ShapeDtypeStruct((keys, pieces[0].shape[1]), BF16)
    return pl.pallas_call(
        functools.partial(attention_kernel, wide, heads, odd, pick, factor, rows, tile, passes),
        out_shape=(out, kept) if passes else out,
        in_specs=[VMEM_SPEC] * 4 + [ANY_SPEC if passes else HBM_SPEC] * len(pieces),
        out_specs=(VMEM_SPEC, HBM_SPEC) if passes else VMEM_SPEC,
        scratch_shapes=[
            pltpu.VMEM((keys, pieces[0].shape[1]), BF16),
            pltpu.VMEM((tok, heads * width), BF16),
            pltpu.VMEM((keys, heads * (width + LANES)), BF16),
            pltpu.VMEM((2, rows, keys), F32),
            pltpu.VMEM((2, rows, LANES), F32),
            pltpu.VMEM((rows, LANES), F32),
            pltpu.VMEM((rows, LANES), F32),
            pltpu.SemaphoreType.DMA((max(len(pieces), keys // tile) + 1,)),
        ],
        compiler_params=pltpu.CompilerParams(vmem_limit_bytes=60 * 2**20),
        cost_estimate=pl.CostEstimate(flops=2 * tok * keys * heads * (width + LANES), bytes_accessed=keys * 1024, transcendentals=0),
    )(query, *tables, weights, *pieces)


def base_kernel(n, heads, first, *refs):
    xs, weights = refs[:heads], refs[heads : heads + n]
    o_ref, w_scr, sems = refs[heads + n :]
    depth = weights[0].shape[0] // heads
    total = o_ref.shape[0]
    parts = [w.at[pl.ds(h * depth, depth)] for h in range(heads) for w in weights]
    for copy in gather_in(parts, w_scr, [i * depth for i in range(heads * n)], sems):
        copy.wait()
    rows = 320 if total % 320 == 0 else total

    def multiply(i, c):
        r = pl.multiple_of(i * rows, rows)
        out = None
        for h, x_ref in enumerate(xs):
            part = jnp.dot(
                x_ref[pl.ds(first + r, rows), :],
                w_scr[h * n * depth : (h + 1) * n * depth, :],
                preferred_element_type=F32,
            )
            out = part if out is None else out + part
        o_ref[pl.ds(r, rows), :] = out.astype(BF16)
        return c

    lax.fori_loop(0, total // rows, multiply, 0)


def project_base(xs, weights, first, total):
    n, heads = len(weights), len(xs)
    depth, width = weights[0].shape
    return pl.pallas_call(
        functools.partial(base_kernel, n, heads, first),
        out_shape=jax.ShapeDtypeStruct((total, width), BF16),
        in_specs=[VMEM_SPEC] * heads + [HBM_SPEC] * n,
        out_specs=VMEM_SPEC,
        scratch_shapes=[
            pltpu.VMEM((n * depth, width), BF16),
            pltpu.SemaphoreType.DMA((heads * n,)),
        ],
        compiler_params=pltpu.CompilerParams(vmem_limit_bytes=20 * 2**20),
        cost_estimate=pl.CostEstimate(flops=2 * total * n * depth * width, bytes_accessed=10**6, transcendentals=0),
        name="project_base",
    )(*xs, *weights)


def norm_kernel(n, s_ref, *refs):
    bases, (x_ref, g_ref) = refs[:2], refs[2:4]
    weights, residuals = refs[4 : 4 + n], refs[4 + n : 4 + 2 * n]
    a_ref, out_ref, edge_ref, o_ref, w_scr, r_scr, y_scr, sems, sems_r, sems_o = refs[4 + 2 * n :]
    depth = weights[0].shape[0]
    total, width = bases[0].shape
    copies = gather_in(weights, w_scr, [i * depth for i in range(n)], sems)
    more = gather_in(residuals, r_scr, [i * 2 * total for i in range(n)], sems_r)
    for copy in copies + more:
        copy.wait()
    rows = 128 if total % 128 == 0 else total
    own = r_scr.shape[1]
    mine = pl.ds(pl.multiple_of(s_ref[n], own), own)

    def put(i):
        at = pl.ds(pl.multiple_of(i * rows, rows), rows)
        return pltpu.make_async_copy(o_ref.at[at], out_ref.at[at], sems_o.at[i])

    for half, b_ref in enumerate(bases):

        def multiply(i, c, half=half, b_ref=b_ref):
            r = pl.multiple_of(i * rows, rows)
            at = pl.multiple_of(half * total + r, rows)
            for p in range(n):
                lanes = pl.ds(pl.multiple_of(s_ref[p], own), own)
                res = r_scr[pl.ds(pl.multiple_of(p * 2 * total + at, rows), rows), :]
                y_scr[:, lanes] = res.astype(F32)
            y = b_ref[pl.ds(r, rows), :].astype(F32) + jnp.dot(
                x_ref[pl.ds(at, rows), :], w_scr[...], preferred_element_type=F32
            )
            y = (y + y_scr[...]).astype(BF16).astype(F32)
            y_scr[...] = y

            @pl.when(s_ref[n + 1] == half)
            def _():
                a_ref[pl.ds(r, rows), :] = y_scr[:, mine].astype(BF16)

            mean = jnp.sum(y * y, axis=1, keepdims=True) * (1.0 / width)
            o_ref[pl.ds(at, rows), :] = (y * lax.rsqrt(mean + epsilon) * g_ref[...]).astype(BF16)
            put(half * (total // rows) + i).start()
            return c

        lax.fori_loop(0, total // rows, multiply, 0)
    edge_ref[0:16, :] = o_ref[0:16, :]
    edge_ref[16:32, :] = o_ref[2 * total - 16 : 2 * total, :]
    for i in range(2 * total // rows):
        put(i).wait()


def project_norm(places, bases, x, gain, weights, residuals):
    total, width = bases[0].shape
    n = len(weights)
    own = residuals[0].shape[1]
    rows = 128 if total % 128 == 0 else total
    return pl.pallas_call(
        functools.partial(norm_kernel, n),
        out_shape=(
            jax.ShapeDtypeStruct((total, own), BF16),
            jax.ShapeDtypeStruct((2 * total, width), BF16),
            jax.ShapeDtypeStruct((32, width), BF16),
        ),
        in_specs=[SMEM_SPEC] + [VMEM_SPEC] * 4 + [HBM_SPEC] * (2 * n),
        out_specs=(VMEM_SPEC, HBM_SPEC, VMEM_SPEC),
        scratch_shapes=[
            pltpu.VMEM((2 * total, width), BF16),
            pltpu.VMEM((n * weights[0].shape[0], width), BF16),
            pltpu.VMEM((n * 2 * total, own), BF16),
            pltpu.VMEM((rows, width), F32),
            pltpu.SemaphoreType.DMA((n,)),
            pltpu.SemaphoreType.DMA((n,)),
            pltpu.SemaphoreType.DMA((2 * total // rows,)),
        ],
        compiler_params=pltpu.CompilerParams(vmem_limit_bytes=28 * 2**20),
        cost_estimate=pl.CostEstimate(flops=4 * total * n * weights[0].shape[0] * width, bytes_accessed=10**6, transcendentals=0),
        name="project_norm",
    )(places, *bases, x, gain, *weights, *residuals)


def up_kernel(half, n, s_ref, in_ref, edge_ref, t_ref, *refs):
    pieces = refs[:n]
    o_ref, x_ref, w_scr, u_scr, e_scr, sems, sems_x = refs[n:]
    block = pieces[0].shape[0]
    copies = gather_in(pieces, w_scr, [pl.multiple_of(s_ref[i], block) for i in range(n)], sems)
    total = x_ref.shape[0]
    rows = 256 if total % 256 == 0 else total

    def take(i):
        at = pl.ds(pl.multiple_of(i * rows, rows), rows)
        return pltpu.make_async_copy(in_ref.at[at], x_ref.at[at], sems_x.at[i])

    for i in range(total // rows):
        take(i).start()
    for copy in copies:
        copy.wait()
    part = 64
    per, last = rows // part, total // part - 1
    e_scr[...] = (
        jnp.dot(edge_ref[...], w_scr[...], preferred_element_type=F32).astype(BF16).astype(F32)
    )
    row = lax.broadcasted_iota(jnp.int32, (part, 2 * half), 0)

    def multiply(i):
        take(i).wait()
        r = pl.multiple_of(i * rows, rows)
        u_scr[pl.ds(r, rows), :] = jnp.dot(
            x_ref[pl.ds(r, rows), :], w_scr[...], preferred_element_type=F32
        ).astype(BF16)

    def mix(i):
        r = pl.multiple_of(i * part, part)
        cur = u_scr[pl.ds(r, part), :].astype(F32)
        up_at = pl.multiple_of(jnp.maximum(r - 16, 0), 16)
        down_at = pl.multiple_of(jnp.minimum(r + part, total - 16), 16)
        above = u_scr[pl.ds(up_at, 16), :].astype(F32)[15:16]
        below = u_scr[pl.ds(down_at, 16), :].astype(F32)[0:1]
        above = jnp.where(i == 0, e_scr[0:1, :], above)
        below = jnp.where(i == last, e_scr[1:2, :], below)
        before = jnp.where(row == 0, above, pltpu.roll(cur, 1, 0))
        after = jnp.where(row == part - 1, below, pltpu.roll(cur, part - 1, 0))
        smooth = t_ref[0:1, :] * before + t_ref[1:2, :] * cur + t_ref[2:3, :] * after
        gate = smooth[:, :half]
        o_ref[pl.ds(r, part), :] = (gate / (1.0 + jnp.exp(-gate)) * smooth[:, half:]).astype(BF16)

    multiply(0)
    if total // rows > 1:
        multiply(1)
        for j in range(per - 1):
            mix(j)

    def step(i, c):
        multiply(i)
        for j in range(per):
            mix((i - 1) * per - 1 + j)
        return c

    lax.fori_loop(2, total // rows, step, 0)

    def rest(i, c):
        mix(i)
        return c

    lax.fori_loop(max(total // rows - 1, 0) * per - (1 if total // rows > 1 else 0), last + 1, rest, 0)


def up_and_mix(places, normed, edge, taps, pieces):
    total, width = normed.shape
    columns = pieces[0].shape[1]
    return pl.pallas_call(
        functools.partial(up_kernel, columns // 2, len(pieces)),
        out_shape=jax.ShapeDtypeStruct((total, columns // 2), BF16),
        in_specs=[SMEM_SPEC, HBM_SPEC] + [VMEM_SPEC] * 2 + [HBM_SPEC] * len(pieces),
        out_specs=VMEM_SPEC,
        scratch_shapes=[
            pltpu.VMEM((total, width), BF16),
            pltpu.VMEM((width, columns), BF16),
            pltpu.VMEM((total, columns), BF16),
            pltpu.VMEM((16, columns), F32),
            pltpu.SemaphoreType.DMA((len(pieces),)),
            pltpu.SemaphoreType.DMA((total // (256 if total % 256 == 0 else total),)),
        ],
        compiler_params=pltpu.CompilerParams(vmem_limit_bytes=60 * 2**20),
        cost_estimate=pl.CostEstimate(flops=2 * total * width * columns, bytes_accessed=10**6, transcendentals=0),
        name="up_and_mix",
    )(places, normed, edge, taps, *pieces)


def down_kernel(n, s_ref, h_ref, *refs):
    pieces = refs[:n]
    keep_ref, send_ref, d_scr, sems = refs[n:]
    block = pieces[0].shape[0]
    copies = gather_in(pieces, d_scr, [pl.multiple_of(s_ref[i], block) for i in range(n)], sems)
    for copy in copies:
        copy.wait()
    far, _, tok, width = keep_ref.shape
    side = s_ref[n]
    rows = tok // 2 if tok % 32 == 0 else tok
    steps = tok // rows

    def multiply(i, c):
        rel = i // steps
        r = pl.multiple_of((i - rel * steps) * rows, rows)
        own = jnp.where(rel == 0, side, 1 - side)
        h = h_ref[pl.ds(pl.multiple_of(own * tok + r, rows), rows), :]
        for o in range(2 * far):
            out = lax.dot_general(
                h,
                d_scr[o * width : (o + 1) * width, :],
                (((1,), (1,)), ((), ())),
                preferred_element_type=F32,
            ).astype(BF16)
            ref = keep_ref if o < far else send_ref
            ref[o % far, rel, pl.ds(r, rows), :] = out
        return c

    lax.fori_loop(0, 2 * steps, multiply, 0)


def down_terms(places, hidden, pieces, tp_size, tok, width):
    shape = jax.ShapeDtypeStruct((tp_size // 2, 2, tok, width), BF16)
    return pl.pallas_call(
        functools.partial(down_kernel, len(pieces)),
        out_shape=(shape, shape),
        in_specs=[SMEM_SPEC, VMEM_SPEC] + [HBM_SPEC] * len(pieces),
        out_specs=(VMEM_SPEC, VMEM_SPEC),
        scratch_shapes=[
            pltpu.VMEM((tp_size * width, hidden.shape[1]), BF16),
            pltpu.SemaphoreType.DMA((len(pieces),)),
        ],
        compiler_params=pltpu.CompilerParams(vmem_limit_bytes=18 * 2**20),
        cost_estimate=pl.CostEstimate(flops=2 * hidden.size * tp_size * width, bytes_accessed=10**6, transcendentals=0),
        name="down_terms",
    )(places, hidden, *pieces)


def per_device(
    sp_size,
    tp_size,
    residual,
    query_wide,
    query_narrow,
    latent,
    rope_key,
    latent_gain,
    expand_wide,
    expand_narrow,
    out_wide,
    out_narrow,
    norm_gain,
    up_gate,
    up_value,
    down_weight,
    conv_taps,
):
    ring = sp_size // 2
    me = lax.axis_index("sp")
    tp = lax.axis_index("tp")
    side = lax.rem(me, 2)
    core = lax.rem(tp, 2)
    tok_rows = residual.shape[0]
    positions = (me * tok_rows + lax.iota(jnp.int32, tok_rows)).astype(jnp.float32)

    def mate(a):
        return lax.ppermute(a, "sp", [(i, i ^ 1) for i in range(sp_size)])

    def along(a, k):
        return lax.ppermute(a, "sp", [(i, (i + 2 * k) % sp_size) for i in range(sp_size)])

    def across(a, bit):
        return lax.ppermute(a, "tp", [(i, i ^ bit) for i in range(tp_size)])

    far_bits = []
    bit = 2
    while bit < tp_size:
        far_bits.append(bit)
        bit *= 2
    tp_order = [0]
    for bit in far_bits + [1]:
        tp_order = tp_order + [p ^ bit for p in tp_order]

    def over_tp(a, axis):
        for bit in far_bits + [1]:
            a = jnp.concatenate([a, across(a, bit)], axis=axis)
        return a

    def spread_tp(a):
        blocks = [a]
        for bit in far_bits + [1]:
            blocks = blocks + [across(b, bit) for b in blocks]
        return blocks

    def paired(own, other):
        return jnp.where(side == 0, jnp.concatenate([own, other]), jnp.concatenate([other, own]))

    latent_float = latent.astype(F32)
    normed_latent = (
        latent_float
        * lax.rsqrt(jnp.mean(latent_float * latent_float, axis=-1, keepdims=True) + epsilon)
        * latent_gain
    ).astype(BF16)
    cosine, sine = angles_of(positions)
    rope_turned = rotate(rope_key, cosine, sine)
    packed = jnp.concatenate([normed_latent, rope_turned, rope_turned], axis=1)
    shares = [bit for bit in (2, 1) if bit < tp_size]
    split_rows = tok_rows // (2 ** len(shares))
    mine = lax.dynamic_slice_in_dim(
        packed, lax.rem(tp, 2 ** len(shares)) * split_rows, split_rows, axis=0
    )
    hops = []
    for _ in range(1, ring):
        hops.append(along(hops[-1] if hops else mine, 1))
    sides = [mate(h) for h in [mine] + hops]
    pieces = [packed]
    for remote in hops + sides:
        group = [remote]
        for bit in shares:
            group = group + [across(g, bit) for g in group]
        pieces = pieces + group

    units = up_gate.shape[1]
    half = units // 2

    def split(a, b):
        low, high = (x[:, :half] for x in (a, b)), (x[:, half:] for x in (a, b))
        low, high = jnp.concatenate(list(low), axis=1), jnp.concatenate(list(high), axis=1)
        return jnp.where(side == 0, low, high), jnp.where(side == 0, high, low)

    up_keep, up_give = split(up_gate, up_value)
    down_keep = jnp.where(side == 0, down_weight[:, :half], down_weight[:, half:])
    down_give = jnp.where(side == 0, down_weight[:, half:], down_weight[:, :half])
    up_a, up_b = [up_keep], [mate(up_give)]
    down_a, down_b = [down_keep], [mate(down_give)]
    for _ in range(1, ring):
        up_a.append(along(up_a[-1], 1))
        up_b.append(along(up_b[-1], 1))
        down_a.append(along(down_a[-1], 1))
        down_b.append(along(down_b[-1], 1))

    outs_w = spread_tp(out_wide)
    outs_n = spread_tp(out_narrow)
    own_width = residual.shape[1]
    pair_residual = paired(residual, mate(residual))
    residuals = spread_tp(pair_residual)
    gains = over_tp(norm_gain[None, :], 1)
    full_gain = jnp.zeros((1, own_width * tp_size), F32)
    lanes_at = []
    for p, q in enumerate(tp_order):
        at = jnp.bitwise_xor(tp, q) * own_width
        lanes_at.append(at)
        piece = slice(p * own_width, (p + 1) * own_width)
        full_gain = lax.dynamic_update_slice_in_dim(full_gain, gains[:, piece], at, axis=1)

    wide_heads = query_wide.shape[1] // (NOPE_W + ROPE)
    narrow_heads = query_narrow.shape[1] // (NOPE_N + ROPE)
    ones, zeros = jnp.ones_like(cosine), jnp.zeros_like(cosine)
    tables_w = (
        jnp.concatenate([cosine, cosine, zeros, zeros], axis=1),
        jnp.concatenate([-sine, sine, zeros, zeros], axis=1),
    )
    tables_n = (
        jnp.concatenate([ones, ones, cosine, cosine], axis=1),
        jnp.concatenate([zeros, zeros, -sine, sine], axis=1),
    )
    heads_w, keys = attend(
        query_wide, tables_w, expand_wide, pieces, wide_heads, True, False,
        (NOPE_W + ROPE) ** (-0.5), passes=True,
    )
    columns = NOPE_N + VAL_N
    heads_n = []
    for h in range(narrow_heads):
        at = slice(h * columns, (h + 1) * columns)
        out = attend(
            query_narrow[:, at], tables_n, expand_narrow[:, at], [keys], 1, False, h % 2 == 1,
            (NOPE_N + ROPE) ** (-0.5),
        )
        if h % 2:
            heads_n[-1] = heads_n[-1] + out
        else:
            heads_n.append(out)
    heads_n = heads_n[0] if len(heads_n) == 1 else jnp.concatenate(heads_n, axis=1)
    heads_n = heads_n[:, : narrow_heads * VAL_N]
    full_w = over_tp(paired(heads_w, mate(heads_w)), 1)
    full_n = over_tp(paired(heads_n, mate(heads_n)), 1)
    lanes_at = jnp.stack(lanes_at + [tp * own_width, side]).astype(jnp.int32)
    bases = []
    for i in range(2):
        bases.append(project_base([full_w], outs_w, i * tok_rows, tok_rows))
    attended, normed, rims = project_norm(lanes_at, bases, full_n, full_gain, outs_n, residuals)

    up_line = [(i, i + 2) for i in range(sp_size - 2)]
    low = lax.ppermute(rims[31:], "sp", up_line)
    high = lax.ppermute(rims[:1], "sp", [(b, a) for a, b in up_line])
    edge = jnp.concatenate([low, high, jnp.zeros((14, normed.shape[1]), BF16)], axis=0)
    block = up_gate.shape[0]
    position = me // 2
    starts, blocks = [], []
    for k in range(ring):
        source = lax.rem(position - k + ring, ring) * 2
        for s in (source + side, source + 1 - side):
            at = s * block
            starts.append(at)
            rel = jnp.bitwise_xor(at // own_width, tp)
            order = lax.rem(rel, 2) * (tp_size // 2) + rel // 2
            blocks.append(order * own_width + lax.rem(at, own_width))
    up_pieces = [p for k in range(ring) for p in (up_a[k], up_b[k])]
    down_pieces = [p for k in range(ring) for p in (down_a[k], down_b[k])]
    taps = jnp.where(side == 0, conv_taps[:, :, :half], conv_taps[:, :, half:]).reshape(3, 2 * half)
    taps = jnp.pad(taps, ((0, 5), (0, 0)))
    hidden = up_and_mix(jnp.stack(starts).astype(jnp.int32), normed, edge, taps, up_pieces)
    kept, sent = down_terms(
        jnp.stack(blocks + [side]).astype(jnp.int32), hidden, down_pieces, tp_size, tok_rows, own_width
    )

    def add(a, b):
        return (a.astype(F32) + b.astype(F32)).astype(BF16)

    terms = add(kept, across(sent, 1))
    for bit in far_bits[:0:-1]:
        n = terms.shape[0] // 2
        terms = add(terms[:n], across(terms[n:], bit))
    cut = tok_rows // 2
    first, second = terms[:, :, :cut], terms[:, :, cut:]
    got_x = across(second[1], 2)
    got_y = mate(first[:, 1])
    more_x = across(add(first[1, 0], got_y[1]), 2)
    more_y = mate(add(second[0, 1], got_x[1]))
    own = attended.astype(F32)
    out_first = own[:cut] + (first[0, 0].astype(F32) + got_y[0].astype(F32) + more_x.astype(F32))
    out_second = own[cut:] + (second[0, 0].astype(F32) + got_x[0].astype(F32) + more_y.astype(F32))
    return jnp.concatenate([out_first, out_second], axis=0).astype(BF16)


def solution(mesh):
    in_specs = (
        P("sp", "tp"),
        P("sp", "tp"),
        P("sp", "tp"),
        P("sp", None),
        P("sp", None),
        P(),
        P(None, "tp"),
        P(None, "tp"),
        P("tp", None),
        P("tp", None),
        P("tp"),
        P("sp", "tp"),
        P("sp", "tp"),
        P("sp", "tp"),
        P(None, None, "tp"),
    )
    out_specs = P("sp", "tp")

    def body(*args):
        return per_device(mesh.shape["sp"], mesh.shape["tp"], *args)

    return jax.shard_map(body, mesh=mesh, in_specs=in_specs, out_specs=out_specs, check_vma=False)
```

```python
import functools

import jax
import jax.numpy as jnp
from jax import lax
from jax.experimental import pallas as pl
from jax.experimental.pallas import tpu as pltpu
from jax.sharding import PartitionSpec as P


ROPE = 64
NOPE_W = 128
VAL_W = 128
NOPE_N = 64
VAL_N = 64
LANES = 128

theta = 10000.0
epsilon = 1e-06
F32 = jnp.float32
BF16 = jnp.bfloat16
LOG2E = 1.4426950408889634


def angles_of(positions):
    half_dim = ROPE // 2
    inverse = jnp.power(jnp.float32(theta), -2.0 * jnp.arange(half_dim, dtype=jnp.float32) / ROPE)
    angles = positions[:, None] * inverse[None, :]
    return jnp.cos(angles), jnp.sin(angles)


def rotate(values, cosine, sine):
    half_dim = values.shape[-1] // 2
    floats = values.astype(jnp.float32)
    lower_half = floats[..., :half_dim]
    upper_half = floats[..., half_dim:]
    turned = jnp.concatenate(
        [
            lower_half * cosine - upper_half * sine,
            lower_half * sine + upper_half * cosine,
        ],
        axis=-1,
    )
    return turned.astype(jnp.bfloat16)


def gather_in(pieces, target, offsets, sems):
    copies = []
    for i, (piece, at) in enumerate(zip(pieces, offsets)):
        copy = pltpu.make_async_copy(piece, target.at[pl.ds(at, piece.shape[0])], sems.at[i])
        copy.start()
        copies.append(copy)
    return copies


def attention_kernel(wide, heads, odd, pick, factor, rows, tile, passes, *refs):
    scratch = 10 if passes else 9
    q_ref, c_ref, n_ref, e_ref, *pieces = refs[:-scratch]
    o_ref, lat, q_scr, kv_ref, s_scr, m_scr, l_scr, a_scr, sems = (refs[-10:-9] + refs[-8:]) if passes else refs[-9:]
    width = q_scr.shape[1] // heads
    blocks = q_ref.shape[0] // rows
    key_count = kv_ref.shape[0]
    rank = e_ref.shape[0]
    tiles = key_count // tile
    groups = tile // LANES
    scale = factor * LOG2E
    value_base = heads * width
    total = heads * blocks

    def fetch(j):
        at = pl.ds(pl.multiple_of(j * tile, tile), tile)
        return pltpu.make_async_copy(pieces[0].at[at], lat.at[at], sems.at[j])

    offsets, at = [], 0
    for piece in pieces:
        offsets.append(at)
        at += piece.shape[0]
    if len(pieces) > 1:
        copies = gather_in(pieces, lat, offsets, sems)
    else:
        copies = []
        for j in range(tiles):
            fetch(j).start()

    def turn(values):
        lane = lax.broadcasted_iota(jnp.int32, values.shape, 1)
        quarter = ROPE // 2
        swapped = jnp.where(
            (lane // quarter) % 2 == 0,
            pltpu.roll(values, LANES - quarter, 1),
            pltpu.roll(values, quarter, 1),
        )
        return (values * c_ref[...] + swapped * n_ref[...]).astype(BF16)

    queries = q_ref[...].astype(F32)
    for h in range(heads):
        if wide:
            head = NOPE_W + ROPE
            full = queries.shape[1]
            if full < 2 * LANES:
                shifted = jnp.concatenate([queries, jnp.zeros((queries.shape[0], 2 * LANES - full), F32)], axis=1)
            else:
                shifted = queries if h + pick == 0 else pltpu.roll(queries, full - (h + pick) * head, 1)
            q_scr[:, h * width : h * width + LANES] = shifted[:, :LANES].astype(BF16)
            q_scr[:, h * width + LANES : (h + 1) * width] = turn(shifted[:, LANES : 2 * LANES])
        else:
            q_scr[:, h * width : (h + 1) * width] = turn(queries[:, h * width : (h + 1) * width])

    for copy in copies:
        copy.wait()
    if passes:
        onward = pltpu.make_async_copy(lat, refs[-9], sems.at[len(pieces)])
        onward.start()

    def expand(j, c):
        at = pl.multiple_of(j * tile, tile)
        if not copies:
            fetch(j).wait()
        x = lat[pl.ds(at, tile), :rank]
        rope = lat[pl.ds(at, tile), rank:].astype(F32)
        lane = lax.broadcasted_iota(jnp.int32, rope.shape, 1)
        for h in range(heads):
            if wide:
                both = NOPE_W + VAL_W
                kv = jnp.dot(x, e_ref[:, (h + pick) * both : (h + pick + 1) * both], preferred_element_type=F32).astype(BF16)
                kv_ref[pl.ds(at, tile), h * width : h * width + LANES] = kv[:, :LANES]
                kv_ref[pl.ds(at, tile), h * width + LANES : (h + 1) * width] = jnp.where(
                    lane < ROPE, rope, 0.0
                ).astype(BF16)
                v_at = value_base + h * LANES
                kv_ref[pl.ds(at, tile), v_at : v_at + LANES] = kv[:, LANES:]
            else:
                kv = jnp.dot(x, e_ref[...], preferred_element_type=F32)
                kv_ref[pl.ds(at, tile), :LANES] = jnp.where(lane < NOPE_N, kv, rope).astype(BF16)
                kv_ref[pl.ds(at, tile), LANES:] = kv.astype(BF16)
        return c

    lax.fori_loop(0, tiles, expand, 0)

    def place(b):
        h = b // blocks
        return h, pl.multiple_of((b - h * blocks) * rows, rows)

    def score(b, buf, j):
        h, r = place(b)
        q = q_scr[pl.ds(r, rows), pl.ds(pl.multiple_of(h * width, LANES), width)]
        at = pl.multiple_of(j * tile, tile)
        k = kv_ref[pl.ds(at, tile), pl.ds(pl.multiple_of(h * width, LANES), width)]
        s = lax.dot_general(q, k, (((1,), (1,)), ((), ())), preferred_element_type=F32)
        s_scr[buf, :, pl.ds(at, tile)] = s
        top = s[:, :LANES]
        for g in range(1, groups):
            top = jnp.maximum(top, s[:, g * LANES : (g + 1) * LANES])
        m_scr[buf] = jnp.maximum(m_scr[buf], top)

    def weigh(b, buf, j):
        h, _ = place(b)
        at = pl.multiple_of(j * tile, tile)
        v_at = pl.multiple_of(value_base + h * LANES, LANES)
        v = kv_ref[pl.ds(at, tile), pl.ds(v_at, LANES)]
        top = m_scr[buf]
        low = []
        part = None
        for g in range(groups):
            s = s_scr[buf, :, pl.ds(pl.multiple_of(at + g * LANES, LANES), LANES)]
            p = jnp.exp2((s - top) * scale)
            part = p if part is None else part + p
            low.append(p.astype(BF16))
        l_scr[...] += part
        a_scr[...] += jnp.dot(jnp.concatenate(low, axis=1), v, preferred_element_type=F32)

    def write(b):
        h, r = place(b)
        out = a_scr[...] / jnp.sum(l_scr[...], axis=1, keepdims=True)
        if not wide:
            lane = lax.broadcasted_iota(jnp.int32, (rows, LANES), 1)
            if odd:
                out = jnp.where(lane >= VAL_N, out, 0.0)
            else:
                out = jnp.where(lane < VAL_N, pltpu.roll(out, VAL_N, 1), 0.0)
        o_ref[pl.ds(r, rows), pl.ds(pl.multiple_of(h * LANES, LANES), LANES)] = out.astype(BF16)

    def clear_max(buf):
        m_scr[buf] = jnp.full((rows, LANES), -jnp.inf, F32)

    clear_max(0)

    def first(j, c):
        score(0, 0, j)
        return c

    lax.fori_loop(0, tiles, first, 0)

    def step(b, c):
        buf = lax.rem(b, 2)
        m_scr[buf] = jnp.broadcast_to(jnp.max(m_scr[buf], axis=1, keepdims=True), (rows, LANES))
        clear_max(1 - buf)
        l_scr[...] = jnp.zeros_like(l_scr)
        a_scr[...] = jnp.zeros_like(a_scr)
        after = jnp.minimum(b + 1, total - 1)

        def both(j, c):
            score(after, 1 - buf, j)
            weigh(b, buf, j)
            return c

        lax.fori_loop(0, tiles, both, 0)
        write(b)
        return c

    lax.fori_loop(0, total, step, 0)
    if passes:
        onward.wait()


VMEM_SPEC = pl.BlockSpec(memory_space=pltpu.VMEM)
SMEM_SPEC = pl.BlockSpec(memory_space=pltpu.SMEM)
HBM_SPEC = pl.BlockSpec(memory_space=pltpu.HBM)
ANY_SPEC = pl.BlockSpec(memory_space=pl.ANY)


def attend(query, tables, weights, pieces, heads, wide, odd, factor, passes=False, pick=0):
    tok = query.shape[0]
    keys = sum(p.shape[0] for p in pieces)
    rows = tok // 2 if tok % 32 == 0 else tok
    tile = 1024 if keys % 1024 == 0 else keys
    width = 2 * LANES if wide else LANES
    out = jax.ShapeDtypeStruct((tok, heads * LANES), BF16)
    kept = jax.ShapeDtypeStruct((keys, pieces[0].shape[1]), BF16)
    row_bytes = 2 * pieces[0].shape[1] + 2 * heads * (width + LANES) + 8 * rows
    grant = keys * row_bytes + 12 * 2**20
    return pl.pallas_call(
        functools.partial(attention_kernel, wide, heads, odd, pick, factor, rows, tile, passes),
        out_shape=(out, kept) if passes else out,
        in_specs=[VMEM_SPEC] * 4 + [ANY_SPEC] * len(pieces),
        out_specs=(VMEM_SPEC, ANY_SPEC) if passes else VMEM_SPEC,
        scratch_shapes=[
            pltpu.VMEM((keys, pieces[0].shape[1]), BF16),
            pltpu.VMEM((tok, heads * width), BF16),
            pltpu.VMEM((keys, heads * (width + LANES)), BF16),
            pltpu.VMEM((2, rows, keys), F32),
            pltpu.VMEM((2, rows, LANES), F32),
            pltpu.VMEM((rows, LANES), F32),
            pltpu.VMEM((rows, LANES), F32),
            pltpu.SemaphoreType.DMA((max(len(pieces), keys // tile) + 1,)),
        ],
        compiler_params=pltpu.CompilerParams(vmem_limit_bytes=max(40 * 2**20, min(62 * 2**20, grant))),
        cost_estimate=pl.CostEstimate(flops=2 * tok * keys * heads * (width + LANES), bytes_accessed=keys * 1024, transcendentals=0),
    )(query, *tables, weights, *pieces)


def base_kernel(n, heads, first, *refs):
    xs, weights = refs[:heads], refs[heads : heads + n]
    o_ref, w_scr, sems = refs[heads + n :]
    depth = weights[0].shape[0] // heads
    total = o_ref.shape[0]
    parts = [w.at[pl.ds(h * depth, depth)] for h in range(heads) for w in weights]
    for copy in gather_in(parts, w_scr, [i * depth for i in range(heads * n)], sems):
        copy.wait()
    rows = 320 if total % 320 == 0 else total

    def multiply(i, c):
        r = pl.multiple_of(i * rows, rows)
        out = None
        for h, x_ref in enumerate(xs):
            part = jnp.dot(
                x_ref[pl.ds(first + r, rows), :],
                w_scr[h * n * depth : (h + 1) * n * depth, :],
                preferred_element_type=F32,
            )
            out = part if out is None else out + part
        o_ref[pl.ds(r, rows), :] = out.astype(BF16)
        return c

    lax.fori_loop(0, total // rows, multiply, 0)


def project_base(xs, weights, first, total):
    n, heads = len(weights), len(xs)
    depth, width = weights[0].shape
    return pl.pallas_call(
        functools.partial(base_kernel, n, heads, first),
        out_shape=jax.ShapeDtypeStruct((total, width), BF16),
        in_specs=[VMEM_SPEC] * heads + [ANY_SPEC] * n,
        out_specs=VMEM_SPEC,
        scratch_shapes=[
            pltpu.VMEM((n * depth, width), BF16),
            pltpu.SemaphoreType.DMA((heads * n,)),
        ],
        compiler_params=pltpu.CompilerParams(vmem_limit_bytes=20 * 2**20),
        cost_estimate=pl.CostEstimate(flops=2 * total * n * depth * width, bytes_accessed=10**6, transcendentals=0),
        name="pb",
    )(*xs, *weights)


def norm_kernel(n, s_ref, *refs):
    base_ref, x_ref, g_ref = refs[:3]
    weights, residuals = refs[3 : 3 + n], refs[3 + n : 3 + 2 * n]
    a_ref, out_ref, edge_ref, o_ref, w_scr, r_scr, y_scr, sems, sems_r, sems_o = refs[3 + 2 * n :]
    depth = weights[0].shape[0]
    total, width = a_ref.shape[0], base_ref.shape[1]
    bases = [base_ref.at[pl.ds(i * total, total)] for i in range(2)]
    copies = gather_in(weights, w_scr, [i * depth for i in range(n)], sems)
    more = gather_in(residuals, r_scr, [i * 2 * total for i in range(n)], sems_r)
    for copy in copies + more:
        copy.wait()
    rows = 128 if total % 128 == 0 else total
    own = r_scr.shape[1]
    mine = pl.ds(pl.multiple_of(s_ref[n], own), own)

    def put(i):
        at = pl.ds(pl.multiple_of(i * rows, rows), rows)
        return pltpu.make_async_copy(o_ref.at[at], out_ref.at[at], sems_o.at[i])

    for half, b_ref in enumerate(bases):

        def multiply(i, c, half=half, b_ref=b_ref):
            r = pl.multiple_of(i * rows, rows)
            at = pl.multiple_of(half * total + r, rows)
            for p in range(n):
                lanes = pl.ds(pl.multiple_of(s_ref[p], own), own)
                res = r_scr[pl.ds(pl.multiple_of(p * 2 * total + at, rows), rows), :]
                y_scr[:, lanes] = res.astype(F32)
            y = b_ref[pl.ds(r, rows), :].astype(F32) + jnp.dot(
                x_ref[pl.ds(at, rows), :], w_scr[...], preferred_element_type=F32
            )
            y = (y + y_scr[...]).astype(BF16).astype(F32)
            y_scr[...] = y

            @pl.when(s_ref[n + 1] == half)
            def _():
                a_ref[pl.ds(r, rows), :] = y_scr[:, mine].astype(BF16)

            mean = jnp.sum(y * y, axis=1, keepdims=True) * (1.0 / width)
            o_ref[pl.ds(at, rows), :] = (y * lax.rsqrt(mean + epsilon) * g_ref[...]).astype(BF16)
            put(half * (total // rows) + i).start()
            return c

        lax.fori_loop(0, total // rows, multiply, 0)
    edge_ref[0:16, :] = o_ref[0:16, :]
    edge_ref[16:32, :] = o_ref[2 * total - 16 : 2 * total, :]
    for i in range(2 * total // rows):
        put(i).wait()


def project_norm(places, base, x, gain, weights, residuals):
    total, width = base.shape[0] // 2, base.shape[1]
    n = len(weights)
    own = residuals[0].shape[1]
    rows = 128 if total % 128 == 0 else total
    return pl.pallas_call(
        functools.partial(norm_kernel, n),
        out_shape=(
            jax.ShapeDtypeStruct((total, own), BF16),
            jax.ShapeDtypeStruct((2 * total, width), BF16),
            jax.ShapeDtypeStruct((32, width), BF16),
        ),
        in_specs=[SMEM_SPEC] + [VMEM_SPEC] * 3 + [ANY_SPEC] * (2 * n),
        out_specs=(VMEM_SPEC, HBM_SPEC, VMEM_SPEC),
        scratch_shapes=[
            pltpu.VMEM((2 * total, width), BF16),
            pltpu.VMEM((n * weights[0].shape[0], width), BF16),
            pltpu.VMEM((n * 2 * total, own), BF16),
            pltpu.VMEM((rows, width), F32),
            pltpu.SemaphoreType.DMA((n,)),
            pltpu.SemaphoreType.DMA((n,)),
            pltpu.SemaphoreType.DMA((2 * total // rows,)),
        ],
        compiler_params=pltpu.CompilerParams(vmem_limit_bytes=28 * 2**20),
        cost_estimate=pl.CostEstimate(flops=4 * total * n * weights[0].shape[0] * width, bytes_accessed=10**6, transcendentals=0),
        name="pn",
    )(places, base, x, gain, *weights, *residuals)


def up_kernel(half, n, s_ref, in_ref, edge_ref, t_ref, *refs):
    pieces = refs[:n]
    o_ref, x_scr, w_scr, u_scr, sems, sems_x = refs[n:]
    block = pieces[0].shape[0]
    copies = gather_in(pieces, w_scr, [pl.multiple_of(s_ref[i], block) for i in range(n)], sems)
    total = in_ref.shape[0]
    rows = 256 if total % 256 == 0 else total
    rim = edge_ref.shape[0]

    def take(i):
        at = pl.multiple_of(i * rows, rows)
        to = pl.multiple_of(at + rim, rim)
        return pltpu.make_async_copy(in_ref.at[pl.ds(at, rows)], x_scr.at[pl.ds(to, rows)], sems_x.at[i])

    for i in range(total // rows):
        take(i).start()
    x_scr[:rim, :] = edge_ref[...]
    for copy in copies:
        copy.wait()
    part = 64
    per, last = rows // part, total // part - 1
    row = lax.broadcasted_iota(jnp.int32, (part, 2 * half), 0)

    def multiply(i):
        take(i).wait()
        first = isinstance(i, int) and i == 0
        at = pl.ds(0, rows + rim) if first else pl.ds(pl.multiple_of(i * rows + rim, rim), rows)
        u_scr[at, :] = jnp.dot(x_scr[at, :], w_scr[...], preferred_element_type=F32).astype(BF16)

    def mix(i):
        r = pl.multiple_of(i * part, part)
        cur = u_scr[pl.ds(pl.multiple_of(r + rim, rim), part), :].astype(F32)
        down_at = pl.multiple_of(jnp.where(i == last, 0, r + part + rim), rim)
        above = u_scr[pl.ds(pl.multiple_of(r, rim), rim), :].astype(F32)[rim - 1 :]
        below = u_scr[pl.ds(down_at, rim), :].astype(F32)[:1]
        before = jnp.where(row == 0, above, pltpu.roll(cur, 1, 0))
        after = jnp.where(row == part - 1, below, pltpu.roll(cur, part - 1, 0))
        smooth = t_ref[0:1, :] * before + t_ref[1:2, :] * cur + t_ref[2:3, :] * after
        gate = smooth[:, :half]
        o_ref[pl.ds(r, part), :] = (gate / (1.0 + jnp.exp(-gate)) * smooth[:, half:]).astype(BF16)

    multiply(0)
    if total // rows > 1:
        multiply(1)
        for j in range(per - 1):
            mix(j)

    def step(i, c):
        multiply(i)
        for j in range(per):
            mix((i - 1) * per - 1 + j)
        return c

    lax.fori_loop(2, total // rows, step, 0)

    def rest(i, c):
        mix(i)
        return c

    lax.fori_loop(max(total // rows - 1, 0) * per - (1 if total // rows > 1 else 0), last + 1, rest, 0)


def up_and_mix(places, normed, edge, taps, pieces):
    total, width = normed.shape
    columns = pieces[0].shape[1]
    return pl.pallas_call(
        functools.partial(up_kernel, columns // 2, len(pieces)),
        out_shape=jax.ShapeDtypeStruct((total, columns // 2), BF16),
        in_specs=[SMEM_SPEC, HBM_SPEC] + [VMEM_SPEC] * 2 + [HBM_SPEC] * len(pieces),
        out_specs=VMEM_SPEC,
        scratch_shapes=[
            pltpu.VMEM((total + 16, width), BF16),
            pltpu.VMEM((width, columns), BF16),
            pltpu.VMEM((total + 16, columns), BF16),
            pltpu.SemaphoreType.DMA((len(pieces),)),
            pltpu.SemaphoreType.DMA((total // (256 if total % 256 == 0 else total),)),
        ],
        compiler_params=pltpu.CompilerParams(vmem_limit_bytes=60 * 2**20),
        cost_estimate=pl.CostEstimate(flops=2 * total * width * columns, bytes_accessed=10**6, transcendentals=0),
        name="mx",
    )(places, normed, edge, taps, *pieces)


def down_kernel(n, base, s_ref, h_ref, *refs):
    pieces = refs[:n]
    o_ref, d_scr, sems = refs[n:]
    block = pieces[0].shape[0]
    copies = gather_in(pieces, d_scr, [pl.multiple_of(s_ref[i], block) for i in range(n)], sems)
    for copy in copies:
        copy.wait()
    far, _, tok, width = o_ref.shape
    side = s_ref[n]
    rows = tok // 2 if tok % 32 == 0 else tok
    steps = tok // rows

    def multiply(i, c):
        rel = i // steps
        r = pl.multiple_of((i - rel * steps) * rows, rows)
        own = jnp.where(rel == 0, side, 1 - side)
        h = h_ref[pl.ds(pl.multiple_of(own * tok + r, rows), rows), :]
        for o in range(far):
            at = (base + o) * width
            o_ref[o, rel, pl.ds(r, rows), :] = lax.dot_general(
                h, d_scr[at : at + width, :], (((1,), (1,)), ((), ())), preferred_element_type=F32
            ).astype(BF16)
        return c

    lax.fori_loop(0, 2 * steps, multiply, 0)


def down_terms(places, hidden, pieces, tp_size, tok, width, base):
    far = tp_size // 2
    return pl.pallas_call(
        functools.partial(down_kernel, len(pieces), base),
        out_shape=jax.ShapeDtypeStruct((far, 2, tok, width), BF16),
        in_specs=[SMEM_SPEC, VMEM_SPEC] + [HBM_SPEC] * len(pieces),
        out_specs=VMEM_SPEC,
        scratch_shapes=[
            pltpu.VMEM((tp_size * width, hidden.shape[1]), BF16),
            pltpu.SemaphoreType.DMA((len(pieces),)),
        ],
        compiler_params=pltpu.CompilerParams(vmem_limit_bytes=18 * 2**20),
        cost_estimate=pl.CostEstimate(flops=hidden.size * tp_size * width, bytes_accessed=10**6, transcendentals=0),
        name="dt",
    )(places, hidden, *pieces)


def per_device(
    sp_size,
    tp_size,
    residual,
    query_wide,
    query_narrow,
    latent,
    rope_key,
    latent_gain,
    expand_wide,
    expand_narrow,
    out_wide,
    out_narrow,
    norm_gain,
    up_gate,
    up_value,
    down_weight,
    conv_taps,
):
    ring = sp_size // 2
    me = lax.axis_index("sp")
    tp = lax.axis_index("tp")
    side = lax.rem(me, 2)
    core = lax.rem(tp, 2)
    tok_rows = residual.shape[0]
    positions = (me * tok_rows + lax.iota(jnp.int32, tok_rows)).astype(jnp.float32)

    def mate(a):
        return lax.ppermute(a, "sp", [(i, i ^ 1) for i in range(sp_size)])

    def along(a, k):
        return lax.ppermute(a, "sp", [(i, (i + 2 * k) % sp_size) for i in range(sp_size)])

    def across(a, bit):
        return lax.ppermute(a, "tp", [(i, i ^ bit) for i in range(tp_size)])

    far_bits = []
    bit = 2
    while bit < tp_size:
        far_bits.append(bit)
        bit *= 2
    tp_order = [0]
    for bit in far_bits + [1]:
        tp_order = tp_order + [p ^ bit for p in tp_order]

    def over_tp(a, axis):
        for bit in far_bits + [1]:
            a = jnp.concatenate([a, across(a, bit)], axis=axis)
        return a

    def spread_tp(a):
        blocks = [a]
        for bit in far_bits + [1]:
            blocks = blocks + [across(b, bit) for b in blocks]
        return blocks

    def paired(own, other):
        return jnp.where(side == 0, jnp.concatenate([own, other]), jnp.concatenate([other, own]))

    latent_float = latent.astype(F32)
    normed_latent = (
        latent_float
        * lax.rsqrt(jnp.mean(latent_float * latent_float, axis=-1, keepdims=True) + epsilon)
        * latent_gain
    ).astype(BF16)
    cosine, sine = angles_of(positions)
    rope_turned = rotate(rope_key, cosine, sine)
    packed = jnp.concatenate([normed_latent, rope_turned, rope_turned], axis=1)
    shares = [bit for bit in (2, 1) if bit < tp_size]
    split_rows = tok_rows // (2 ** len(shares))
    mine = lax.dynamic_slice_in_dim(
        packed, lax.rem(tp, 2 ** len(shares)) * split_rows, split_rows, axis=0
    )
    hops = []
    for _ in range(1, ring):
        hops.append(along(hops[-1] if hops else mine, 1))
    sides = [mate(h) for h in [mine] + hops]
    pieces = [packed]
    for remote in hops + sides:
        group = [remote]
        for bit in shares:
            group = group + [across(g, bit) for g in group]
        pieces = pieces + group

    units = up_gate.shape[1]
    half = units // 2

    def split(a, b):
        low, high = (x[:, :half] for x in (a, b)), (x[:, half:] for x in (a, b))
        low, high = jnp.concatenate(list(low), axis=1), jnp.concatenate(list(high), axis=1)
        return jnp.where(side == 0, low, high), jnp.where(side == 0, high, low)

    up_keep, up_give = split(up_gate, up_value)
    down_keep = jnp.where(side == 0, down_weight[:, :half], down_weight[:, half:])
    down_give = jnp.where(side == 0, down_weight[:, half:], down_weight[:, :half])
    up_a, up_b = [up_keep], [mate(up_give)]
    down_a, down_b = [down_keep], [mate(down_give)]
    for _ in range(1, ring):
        up_a.append(along(up_a[-1], 1))
        up_b.append(along(up_b[-1], 1))
        down_a.append(along(down_a[-1], 1))
        down_b.append(along(down_b[-1], 1))

    outs_w = spread_tp(out_wide)
    outs_n = spread_tp(out_narrow)
    own_width = residual.shape[1]
    pair_residual = paired(residual, mate(residual))
    residuals = spread_tp(pair_residual)
    gains = over_tp(norm_gain[None, :], 1)
    full_gain = jnp.zeros((1, own_width * tp_size), F32)
    lanes_at = []
    for p, q in enumerate(tp_order):
        at = jnp.bitwise_xor(tp, q) * own_width
        lanes_at.append(at)
        piece = slice(p * own_width, (p + 1) * own_width)
        full_gain = lax.dynamic_update_slice_in_dim(full_gain, gains[:, piece], at, axis=1)

    wide_heads = query_wide.shape[1] // (NOPE_W + ROPE)
    narrow_heads = query_narrow.shape[1] // (NOPE_N + ROPE)
    ones, zeros = jnp.ones_like(cosine), jnp.zeros_like(cosine)
    tables_w = (
        jnp.concatenate([cosine, cosine, zeros, zeros], axis=1),
        jnp.concatenate([-sine, sine, zeros, zeros], axis=1),
    )
    tables_n = (
        jnp.concatenate([ones, ones, cosine, cosine], axis=1),
        jnp.concatenate([zeros, zeros, -sine, sine], axis=1),
    )
    heads_w, keys = attend(
        query_wide, tables_w, expand_wide, pieces, wide_heads, True, False,
        (NOPE_W + ROPE) ** (-0.5), passes=True,
    )
    columns = NOPE_N + VAL_N
    heads_n = []
    for h in range(narrow_heads):
        at = slice(h * columns, (h + 1) * columns)
        out = attend(
            query_narrow[:, at], tables_n, expand_narrow[:, at], [keys], 1, False, h % 2 == 1,
            (NOPE_N + ROPE) ** (-0.5),
        )
        if h % 2:
            heads_n[-1] = heads_n[-1] + out
        else:
            heads_n.append(out)
    heads_n = heads_n[0] if len(heads_n) == 1 else jnp.concatenate(heads_n, axis=1)
    heads_n = heads_n[:, : narrow_heads * VAL_N]
    full_w = over_tp(paired(heads_w, mate(heads_w)), 1)
    full_n = over_tp(paired(heads_n, mate(heads_n)), 1)
    lanes_at = jnp.stack(lanes_at + [tp * own_width, side]).astype(jnp.int32)
    base = project_base([full_w], outs_w, 0, 2 * tok_rows)
    attended, normed, rims = project_norm(lanes_at, base, full_n, full_gain, outs_n, residuals)

    up_line = [(i, i + 2) for i in range(sp_size - 2)]
    low = lax.ppermute(rims[31:], "sp", up_line)
    high = lax.ppermute(rims[:1], "sp", [(b, a) for a, b in up_line])
    edge = jnp.concatenate([high, jnp.zeros((14, normed.shape[1]), BF16), low], axis=0)
    block = up_gate.shape[0]
    position = me // 2
    starts, blocks = [], []
    for k in range(ring):
        source = lax.rem(position - k + ring, ring) * 2
        for s in (source + side, source + 1 - side):
            at = s * block
            starts.append(at)
            rel = jnp.bitwise_xor(at // own_width, tp)
            order = lax.rem(rel, 2) * (tp_size // 2) + rel // 2
            blocks.append(order * own_width + lax.rem(at, own_width))
    up_pieces = [p for k in range(ring) for p in (up_a[k], up_b[k])]
    down_pieces = [p for k in range(ring) for p in (down_a[k], down_b[k])]
    taps = jnp.where(side == 0, conv_taps[:, :, :half], conv_taps[:, :, half:]).reshape(3, 2 * half)
    taps = jnp.pad(taps, ((0, 5), (0, 0)))
    hidden = up_and_mix(jnp.stack(starts).astype(jnp.int32), normed, edge, taps, up_pieces)
    at = jnp.stack(blocks + [side]).astype(jnp.int32)
    sent = down_terms(at, hidden, down_pieces, tp_size, tok_rows, own_width, tp_size // 2)
    kept = down_terms(at, hidden, down_pieces, tp_size, tok_rows, own_width, 0)

    def add(a, b):
        return (a.astype(F32) + b.astype(F32)).astype(BF16)

    terms = add(kept, across(sent, 1))
    for bit in far_bits[:0:-1]:
        n = terms.shape[0] // 2
        terms = add(terms[:n], across(terms[n:], bit))
    cut = tok_rows // 2
    first, second = terms[:, :, :cut], terms[:, :, cut:]
    got_x = across(second[1], 2)
    got_y = mate(first[:, 1])
    more_x = across(add(first[1, 0], got_y[1]), 2)
    more_y = mate(add(second[0, 1], got_x[1]))
    own = attended.astype(F32)
    out_first = own[:cut] + (first[0, 0].astype(F32) + got_y[0].astype(F32) + more_x.astype(F32))
    out_second = own[cut:] + (second[0, 0].astype(F32) + got_x[0].astype(F32) + more_y.astype(F32))
    return jnp.concatenate([out_first, out_second], axis=0).astype(BF16)


def solution(mesh):
    in_specs = (
        P("sp", "tp"),
        P("sp", "tp"),
        P("sp", "tp"),
        P("sp", None),
        P("sp", None),
        P(),
        P(None, "tp"),
        P(None, "tp"),
        P("tp", None),
        P("tp", None),
        P("tp"),
        P("sp", "tp"),
        P("sp", "tp"),
        P("sp", "tp"),
        P(None, None, "tp"),
    )
    out_specs = P("sp", "tp")

    def body(*args):
        return per_device(mesh.shape["sp"], mesh.shape["tp"], *args)

    return jax.shard_map(body, mesh=mesh, in_specs=in_specs, out_specs=out_specs, check_vma=False)
```
